32 devices in a mesh: grp: 2 (over x), tp: 16 (over z, y, core).
Axes of the slice: x: 2, y: 2, z: 4, core: 2. Of those that a mesh axis runs over, the one named last changes fastest.
Arguments:
- tokens: bfloat16 [2048, 2048], P('grp', 'tp'), parts along dimension 0, may hold values from -8 to 8
- carried: float32 [2, 2, 32, 64, 2048], P(None, None, 'tp', None, 'grp'), parts along dimension 4, may hold values from -3 to 3
- proj_in: bfloat16 [2, 2048, 512], P(None, None, 'tp'), may hold values from -0.125 to 0.125
- proj_gate: bfloat16 [2, 2048, 512], P(None, None, 'tp'), may hold values from -0.125 to 0.125
- proj_out: bfloat16 [2, 512, 2048], P(None, None, 'tp'), may hold values from -0.5 to 0.5
- norm_params: bfloat16 [2, 2, 2048], P(None, None, 'tp'), may hold values from -0.5 to 2.4
- lambda_re: float32 [2, 32, 64], P(None, 'tp'), may hold values from -1 to -0.05
- lambda_im: float32 [2, 32, 64], P(None, 'tp'), may hold values from -3 to 3
- log_step: float32 [2, 32], P(None, 'tp'), may hold values from -3 to 0
- in_coupling: float32 [2, 2, 32, 64, 16], P(None, None, 'tp'), may hold values from -1 to 1
- out_coupling: float32 [2, 2, 32, 16, 64], P(None, None, 'tp'), may hold values from -1.5 to 1.5
- skip_gain: float32 [2, 512], P(None, 'tp'), may hold values from -4 to 4
Outputs:
- stream_out: bfloat16 [2048, 2048], P('grp', 'tp'), parts along dimension 0
- new_carried: float32 [2, 2, 32, 64, 2048], P(None, None, 'tp', None, 'grp'), parts along dimension 4
The draws below stay inside these ranges and needn't reach their ends.
There are 2 independent parts, one for each index of `grp`. The reference program is written for one: setup_inputs(seed, part) draws one part's arguments, and reference() takes and returns one part's arrays. A program takes and returns all parts, laid end to end along the dimension named above; an argument that names none is the same for every part. Nothing has to cross between parts.
All inputs are finite; a program needn't handle non-finite values.
Results may differ from the reference program's by a relative error of at most 0.015.
Values may be sent and summed in bfloat16 or wider, within the bound.
A program may use at most 64 MiB of HBM per device.

```python
import jax
import jax.numpy as jnp
from jax import lax

D = 2048
GROUPS = 32
GROUP_CH = 16
STATE = 64
SSM = 512
LAYERS = 2
BATCH = 1024


def draw_tokens(key, part):
    keys = jax.random.split(jax.random.fold_in(key, 11), 3)
    base = jax.random.normal(keys[0], (BATCH, D), jnp.float32)
    ramp = jnp.exp(jnp.linspace(jnp.log(0.4), jnp.log(1.6), D)) * jax.random.uniform(keys[1], (D,), jnp.float32, 0.7, 1.3)
    scales = jnp.exp(jax.random.uniform(keys[2], (BATCH, 1), jnp.float32, jnp.log(0.5), jnp.log(2.0)))
    values = base * ramp[None, :] * scales
    return jnp.clip(values, -8.0, 8.0).astype(jnp.bfloat16)


def draw_norm_params(key, part):
    keys = jax.random.split(jax.random.fold_in(key, 23), 2)
    ramp = jnp.exp(jnp.linspace(jnp.log(0.6), jnp.log(1.8), D))
    gains = ramp[None, :] * jax.random.uniform(keys[0], (LAYERS, D), jnp.float32, 0.8, 1.2)
    biases = jax.random.uniform(keys[1], (LAYERS, D), jnp.float32, -0.4, 0.4)
    return jnp.stack([gains, biases], axis=1).astype(jnp.bfloat16)


def steps_of(own_key, extent, pieces, low, top_value):
    factor_of = 1.0
    for dim, shards_of in pieces:
        heights = jax.random.uniform(jax.random.fold_in(jax.random.fold_in(own_key, 6), dim), (shards_of,), jnp.float32, low / len(pieces), top_value / len(pieces))
        factor_of = factor_of * jnp.repeat(jnp.exp(heights), extent[dim] // shards_of).reshape((-1,) + (1,) * (len(extent) - 1 - dim))
    return factor_of


def scatter_about(own_key, shape, spread, reach, cuts=(), held_as=jnp.bfloat16):
    loudness = steps_of(own_key, shape, cuts, -0.22, 0.18) if cuts else 1.0
    array = jax.random.normal(own_key, shape, jnp.float32) * spread * loudness
    return jnp.minimum(jnp.maximum(array, -reach), reach).astype(held_as)


def setup_inputs(seed: int = 0, part: int = 0) -> dict:
    splits = jax.random.split(jax.random.key(seed), 13)
    own_keys = jax.random.split(jax.random.fold_in(splits[12], part), 13)
    tokens = draw_tokens(jax.random.fold_in(jax.random.fold_in(splits[12], part), 71), part)
    carried = scatter_about(own_keys[1], (LAYERS, 2, GROUPS, STATE, BATCH), 0.3, 3.0, ((2, 16),), jnp.float32)
    proj_in = scatter_about(splits[2], (LAYERS, D, SSM), D ** -0.5, 0.125, ((2, 16),))
    proj_gate = scatter_about(splits[3], (LAYERS, D, SSM), D ** -0.5, 0.125, ((2, 16),))
    proj_out = scatter_about(splits[4], (LAYERS, SSM, D), (SSM // 4) ** -0.5, 0.5, ((2, 16),))
    norm_params = draw_norm_params(jax.random.fold_in(splits[12], 71), part)
    lambda_re = jnp.clip(-1.0 + 0.95 * jax.random.uniform(splits[6], (LAYERS, GROUPS, STATE), jnp.float32) ** steps_of(splits[6], (LAYERS, GROUPS, STATE), ((1, 16),), -0.2, 0.2), -1.0, -0.05)
    lambda_im = jnp.clip(jax.random.uniform(splits[7], (LAYERS, GROUPS, STATE), jnp.float32, -3.0, 3.0) * steps_of(splits[7], (LAYERS, GROUPS, STATE), ((1, 16),), -0.4, 0.0), -3.0, 3.0)
    log_step = jnp.clip(-3.0 + 3.0 * jax.random.uniform(splits[8], (LAYERS, GROUPS), jnp.float32) ** steps_of(splits[8], (LAYERS, GROUPS), ((1, 16),), -0.2, 0.2), -3.0, 0.0)
    in_coupling = scatter_about(splits[9], (LAYERS, 2, GROUPS, STATE, GROUP_CH), (2 * GROUP_CH) ** -0.5, 1.0, ((2, 16),), jnp.float32)
    out_coupling = scatter_about(splits[10], (LAYERS, 2, GROUPS, GROUP_CH, STATE), (STATE // 4) ** -0.5, 1.5, ((2, 16),), jnp.float32)
    skip_gain = scatter_about(splits[11], (LAYERS, SSM), 1.0, 4.0, ((1, 16),), jnp.float32)
    return dict(tokens=tokens, carried=carried, proj_in=proj_in, proj_gate=proj_gate, proj_out=proj_out, norm_params=norm_params, lambda_re=lambda_re, lambda_im=lambda_im, log_step=log_step, in_coupling=in_coupling, out_coupling=out_coupling, skip_gain=skip_gain)


residual_scale = 1.4142135623730951
norm_eps = 1e-05
highest_precision = lax.Precision.HIGHEST

def discretize(lam_re, lam_im, log_dt, coupling):
    step_len = jnp.exp(log_dt)[:, None]
    modulus = jnp.exp(lam_re * step_len)
    decay_re = modulus * jnp.cos(lam_im * step_len)
    decay_im = modulus * jnp.sin(lam_im * step_len)
    denominator = lam_re * lam_re + lam_im * lam_im
    shifted = decay_re - 1.0
    coef_re = (shifted * lam_re + decay_im * lam_im) / denominator
    coef_im = (decay_im * lam_re - shifted * lam_im) / denominator
    in_re = coef_re[..., None] * coupling[0] - coef_im[..., None] * coupling[1]
    in_im = coef_re[..., None] * coupling[1] + coef_im[..., None] * coupling[0]
    return (decay_re, decay_im, in_re, in_im)

def recur(drive, gate_pre, states, lam_re, lam_im, log_dt, in_c, output_coupling, skip_connection):
    channel_groups = lam_re.shape[0]
    batch_rows = drive.shape[0]
    drive_expanded = drive.astype(jnp.float32).reshape(batch_rows, channel_groups, -1)
    decay_re, decay_im, in_re, in_im = discretize(lam_re, lam_im, log_dt, in_c)
    push_re = jnp.einsum('bgc,gpc->gpb', drive_expanded, in_re, precision=highest_precision)
    push_im = jnp.einsum('bgc,gpc->gpb', drive_expanded, in_im, precision=highest_precision)
    fresh_real = decay_re[..., None] * states[0] - decay_im[..., None] * states[1] + push_re
    fresh_imaginary = decay_re[..., None] * states[1] + decay_im[..., None] * states[0] + push_im
    readout_rows = jnp.einsum('jyn,jmy->njm', fresh_real, output_coupling[0], precision=highest_precision) - jnp.einsum('jyn,jmy->njm', fresh_imaginary, output_coupling[1], precision=highest_precision) + skip_connection.reshape(channel_groups, -1) * drive_expanded
    readout_rows = readout_rows.reshape(batch_rows, -1)
    gated = (jax.nn.gelu(readout_rows) * jax.nn.sigmoid(gate_pre.astype(jnp.float32))).astype(jnp.bfloat16)
    return (gated, jnp.stack([fresh_real, fresh_imaginary]))

def norm_rows(summed, params):
    wide = summed.astype(jnp.float32)
    mean_row = lax.optimization_barrier(jnp.mean(wide, axis=-1, keepdims=True))
    var_row = lax.optimization_barrier(jnp.mean(wide * wide, axis=-1, keepdims=True)) - mean_row * mean_row
    scaled = (wide - mean_row) * lax.rsqrt(var_row + norm_eps)
    return (scaled * params[0].astype(jnp.float32) + params[1].astype(jnp.float32)).astype(jnp.bfloat16)

def reference(tokens, carried, proj_in, proj_gate, proj_out, norm_params, lambda_re, lambda_im, log_step, in_coupling, out_coupling, skip_gain):
    stream = tokens
    new_states = []
    for layer_idx in range(LAYERS):
        drive = jnp.dot(stream, proj_in[layer_idx], preferred_element_type=jnp.float32).astype(jnp.bfloat16)
        gate_pre = jnp.dot(stream, proj_gate[layer_idx], preferred_element_type=jnp.float32).astype(jnp.bfloat16)
        gated, states = recur(drive, gate_pre, carried[layer_idx], lambda_re[layer_idx], lambda_im[layer_idx], log_step[layer_idx], in_coupling[layer_idx], out_coupling[layer_idx], skip_gain[layer_idx])
        mixed = jnp.dot(gated, proj_out[layer_idx], preferred_element_type=jnp.float32)
        summed = (residual_scale * stream.astype(jnp.float32) + mixed).astype(jnp.bfloat16)
        stream = norm_rows(summed, norm_params[layer_idx])
        new_states.append(states)
    return (stream, jnp.stack(new_states))
```

```python
import functools

import jax
import jax.numpy as jnp
from jax import lax
from jax.experimental import pallas as pl
from jax.experimental.pallas import tpu as pltpu
from jax.sharding import PartitionSpec as P

RESIDUAL_SCALE = 1.4142135623730951
NORM_EPS = 1e-05
HIGHEST = lax.Precision.HIGHEST
F32 = jnp.float32
BF16 = jnp.bfloat16


def column(row):
    m = row.shape[1]
    eye = lax.broadcasted_iota(jnp.int32, (m, m), 0) == lax.broadcasted_iota(jnp.int32, (m, m), 1)
    return jnp.sum(jnp.where(eye, jnp.broadcast_to(row, (m, m)), 0.0), axis=1, keepdims=True)


class Gather:
    def __init__(self, buf, send, recv, place, outer):
        self.buf, self.send, self.recv, self.outer = buf, send, recv, outer
        self.z, self.y, self.c = place

    def idx(self, dz, dy, dc):
        z = lax.rem(self.z + dz + self.outer, self.outer)
        y = self.y if dy == 0 else 1 - self.y
        c = self.c if dc == 0 else 1 - self.c
        return (z * 2 + y) * 2 + c

    def copy(self, block, target, slot):
        return pltpu.make_async_remote_copy(
            src_ref=self.buf.at[block],
            dst_ref=self.buf.at[block],
            send_sem=self.send.at[slot],
            recv_sem=self.recv.at[slot],
            device_id={"tp": target},
            device_id_type=pl.DeviceIdType.MESH,
        )

    def out_z(self, dz):
        return self.copy(self.idx(0, 0, 0), self.idx(dz, 0, 0), dz - 1)

    def out_y(self, dz):
        return self.copy(self.idx(-dz, 0, 0), self.idx(0, 1, 0), self.outer - 1 + dz)

    def out_c(self, dz, dy):
        slot = 2 * self.outer - 1 + 2 * dz + dy
        return self.copy(self.idx(-dz, dy, 0), self.idx(0, 0, 1), slot)

    def start(self):
        for dz in range(1, self.outer):
            self.out_z(dz).start()
        self.out_y(0).start()
        self.out_c(0, 0).start()

    def arrive(self, dz, dy):
        if dy == 1:
            self.copy(self.idx(-dz, 1, 0), self.idx(0, 1, 0), self.outer - 1 + dz).wait_recv()
            self.out_c(dz, 1).start()
        elif dz > 0:
            self.copy(self.idx(-dz, 0, 0), self.idx(-dz, 0, 0), dz - 1).wait_recv()
            self.out_y(dz).start()
            self.out_c(dz, 0).start()

    def ready(self, dz, dy):
        slot = 2 * self.outer - 1 + 2 * dz + dy
        self.copy(self.idx(-dz, dy, 1), self.idx(0, 0, 1), slot).wait_recv()

    def sent(self):
        for dz in range(1, self.outer):
            self.out_z(dz).wait_send()
        for dz in range(self.outer):
            self.out_y(dz).wait_send()
            for dy in range(2):
                self.out_c(dz, dy).wait_send()

    def events(self):
        return [(dz, dy) for dz in range(self.outer) for dy in range(2)]

    def finish(self):
        for event in self.events():
            self.arrive(*event)
        for event in self.events():
            self.ready(*event)


def exchange(buf, send, recv, me, n, shift):
    return pltpu.make_async_remote_copy(
        src_ref=buf.at[me],
        dst_ref=buf.at[me],
        send_sem=send.at[shift - 1],
        recv_sem=recv.at[shift - 1],
        device_id={"tp": lax.rem(me + shift, n)},
        device_id_type=pl.DeviceIdType.MESH,
    )


def received(buf, send, recv, me, n, shift):
    block = lax.rem(me - shift + n, n)
    return pltpu.make_async_remote_copy(
        src_ref=buf.at[block],
        dst_ref=buf.at[block],
        send_sem=send.at[shift - 1],
        recv_sem=recv.at[shift - 1],
        device_id={"tp": block},
        device_id_type=pl.DeviceIdType.MESH,
    )


def kernel(
    n,
    tokens, carried, proj_in, proj_gate, proj_out, norm_params,
    lam_re, lam_im, log_step, in_c, out_c, skip,
    stream_out, new_carried,
    xg, pg, g1, g2, nb, sb, win, wgate, wcat, pown, states, fresh, acc, decay, bbar, outb,
    gsend, grecv, nsend, nrecv, ssend, srecv, lsem,
):
    me = lax.axis_index("tp")
    outer = n // 4
    place = (me // 4, lax.rem(me // 2, 2), lax.rem(me, 2))
    layers, groups, state = lam_re.shape
    rows, width = tokens.shape
    ssm = proj_out.shape[1]
    own = proj_in.shape[2]
    ch = own // groups

    loads = [
        pltpu.make_async_copy(tokens, xg.at[me], lsem.at[0]),
        pltpu.make_async_copy(proj_out.at[0], pg.at[me], lsem.at[1]),
        pltpu.make_async_copy(norm_params, nb.at[me], lsem.at[2]),
        pltpu.make_async_copy(proj_in, win, lsem.at[3]),
        pltpu.make_async_copy(proj_gate, wgate, lsem.at[4]),
        pltpu.make_async_copy(carried, states, lsem.at[5]),
        pltpu.make_async_copy(proj_out.at[1], pown, lsem.at[6]),
    ]
    for load in loads:
        load.start()
    barrier = pltpu.get_barrier_semaphore()
    for shift in range(1, n):
        pl.semaphore_signal(
            barrier, inc=1, device_id={"tp": lax.rem(me + shift, n)}, device_id_type=pl.DeviceIdType.MESH
        )
    pl.semaphore_wait(barrier, n - 1)

    ga = Gather(xg, gsend.at[0], grecv.at[0], place, outer)
    gp = Gather(pg, gsend.at[1], grecv.at[1], place, outer)
    gg = [Gather(g1, gsend.at[2], grecv.at[2], place, outer), Gather(g2, gsend.at[3], grecv.at[3], place, outer)]
    loads[0].wait()
    ga.start()
    loads[2].wait()
    for shift in range(1, n):
        exchange(nb, nsend, nrecv, me, n, shift).start()
    loads[1].wait()
    gp.start()

    loads[3].wait()
    loads[4].wait()
    for l in range(layers):
        wcat[l] = jnp.concatenate([win[l], wgate[l]], axis=1)
    for l in range(layers):
        for g in range(groups):
            lr = lam_re[l, g : g + 1, :]
            li = lam_im[l, g : g + 1, :]
            step_len = jnp.exp(log_step[l : l + 1, g : g + 1])
            modulus = jnp.exp(lr * step_len)
            d_re = modulus * jnp.cos(li * step_len)
            d_im = modulus * jnp.sin(li * step_len)
            den = lr * lr + li * li
            shifted = d_re - 1.0
            k_re = column((shifted * lr + d_im * li) / den)
            k_im = column((d_im * lr - shifted * li) / den)
            decay[l, g, 0] = column(d_re)
            decay[l, g, 1] = column(d_im)
            bbar[l, g, :state] = k_re * in_c[l, 0, g] - k_im * in_c[l, 1, g]
            bbar[l, g, state:] = k_re * in_c[l, 1, g] + k_im * in_c[l, 0, g]

    def pair_dot(dz, dy, first):
        j = ga.idx(-dz, dy, 0) // 2
        lhs = jnp.concatenate([xg[2 * j], xg[2 * j + 1]], axis=1)
        rhs = wcat[0, pl.ds(pl.multiple_of(j * (2 * width), 2 * width), 2 * width), :]
        part = jnp.dot(lhs, rhs, preferred_element_type=F32)
        if first:
            acc[...] = part
        else:
            acc[...] += part

    events = ga.events()
    for i, event in enumerate(events):
        ga.arrive(*event)
        if i > 0:
            ga.ready(*events[i - 1])
            pair_dot(*events[i - 1], i == 1)
    ga.ready(*events[-1])
    pair_dot(*events[-1], False)

    def mixer(l, gbuf, between):
        pre_t = acc[...].astype(BF16).astype(F32).T
        skip_col = column(skip[l : l + 1, :])
        parts = []
        for g in range(groups):
            drive = pre_t[g * ch : (g + 1) * ch]
            push = jnp.dot(bbar[l, g], drive, precision=HIGHEST, preferred_element_type=F32)
            old_re, old_im = states[l, 0, g], states[l, 1, g]
            d_re, d_im = decay[l, g, 0], decay[l, g, 1]
            new_re = d_re * old_re - d_im * old_im + push[:state]
            new_im = d_re * old_im + d_im * old_re + push[state:]
            fresh[l, 0, g] = new_re
            fresh[l, 1, g] = new_im
            parts.append(
                jnp.dot(out_c[l, 0, g], new_re, precision=HIGHEST, preferred_element_type=F32)
                - jnp.dot(out_c[l, 1, g], new_im, precision=HIGHEST, preferred_element_type=F32)
                + skip_col[g * ch : (g + 1) * ch] * drive
            )
            between(g)
        y = jnp.concatenate(parts, axis=0) if groups > 1 else parts[0]
        gbuf[me] = (jax.nn.gelu(y) * jax.nn.sigmoid(pre_t[own:])).astype(BF16)

    p_events = gp.events()
    for event in p_events[: len(p_events) // 4]:
        gp.arrive(*event)
    loads[5].wait()

    def p_step(g):
        share = len(p_events) // 4
        if g == 0:
            for event in p_events[share : 2 * share]:
                gp.arrive(*event)

    mixer(0, g1, p_step)
    gg[0].start()
    stores = [pltpu.make_async_copy(fresh.at[0], new_carried.at[0], lsem.at[7])]
    stores[0].start()
    for event in p_events[len(p_events) // 4 * 2 :]:
        gp.arrive(*event)
    for event in p_events:
        gp.ready(*event)
    gg[0].finish()
    for shift in range(1, n):
        received(nb, nsend, nrecv, me, n, shift).wait_recv()
    ga.sent()

    chunk = min(rows, 128)

    def row_chunk(r, carry):
        at = pl.ds(pl.multiple_of(r * chunk, chunk), chunk)
        gated = g1[:, :, at].reshape(ssm, chunk).astype(F32).T.astype(BF16)
        total = jnp.zeros((chunk, 1), F32)
        square = jnp.zeros((chunk, 1), F32)
        wide = []
        for j in range(n // 2):
            weights = jnp.concatenate([pg[2 * j], pg[2 * j + 1]], axis=1)
            mixed = jnp.dot(gated, weights, preferred_element_type=F32)
            old = jnp.concatenate([xg[2 * j, at, :], xg[2 * j + 1, at, :]], axis=1)
            summed = (RESIDUAL_SCALE * old.astype(F32) + mixed).astype(BF16)
            s = summed.astype(F32)
            total += jnp.sum(s, axis=1, keepdims=True)
            square += jnp.sum(s * s, axis=1, keepdims=True)
            wide.append(summed)
        mean = total / (n * width)
        var = square / (n * width) - mean * mean
        scale = lax.rsqrt(var + NORM_EPS)
        pre = jnp.zeros((chunk, 2 * own), F32)
        for j in range(n // 2):
            par = jnp.concatenate([nb[2 * j, 0], nb[2 * j + 1, 0]], axis=1).astype(F32)
            out = ((wide[j].astype(F32) - mean) * scale * par[0:1] + par[1:2]).astype(BF16)
            xg[2 * j, at, :] = out[:, :width]
            xg[2 * j + 1, at, :] = out[:, width:]
            pre += jnp.dot(out, wcat[1, 2 * j * width : 2 * (j + 1) * width, :], preferred_element_type=F32)
        acc[at, :] = pre
        return carry

    lax.fori_loop(0, rows // chunk, row_chunk, 0)

    mixer(1, g2, lambda g: None)
    gg[1].start()
    stores.append(pltpu.make_async_copy(fresh.at[1], new_carried.at[1], lsem.at[8]))
    stores[1].start()
    residual_t = RESIDUAL_SCALE * xg[me].astype(F32).T
    gain = column(nb[me, 1].astype(F32)[0:1])
    bias = column(nb[me, 1].astype(F32)[1:2])
    loads[6].wait()
    weights_t = pown[...].astype(F32).T.astype(BF16)
    gg[1].finish()
    mixed_t = jnp.dot(weights_t, g2[...].reshape(ssm, rows), preferred_element_type=F32)
    s = (residual_t + mixed_t).astype(BF16).astype(F32)
    sb[me] = jnp.concatenate([jnp.sum(s, axis=0, keepdims=True), jnp.sum(s * s, axis=0, keepdims=True)], axis=0)
    for shift in range(1, n):
        exchange(sb, ssend, srecv, me, n, shift).start()
    for shift in range(1, n):
        received(sb, ssend, srecv, me, n, shift).wait_recv()
    sums = jnp.sum(sb[...], axis=0) / (n * width)
    mean = sums[0:1]
    scale = lax.rsqrt(sums[1:2] - mean * mean + NORM_EPS)
    outb[...] = ((s - mean) * scale * gain + bias).T.astype(BF16)
    last = pltpu.make_async_copy(outb, stream_out, lsem.at[9])
    last.start()
    for gather in (gp, gg[0], gg[1]):
        gather.sent()
    for shift in range(1, n):
        exchange(nb, nsend, nrecv, me, n, shift).wait_send()
        exchange(sb, ssend, srecv, me, n, shift).wait_send()
    for store in stores:
        store.wait()
    last.wait()


def per_device(n, *args):
    tokens, carried, proj_in, _, proj_out, norm_params, lam_re = args[:7]
    rows, width = tokens.shape
    layers, groups, state = lam_re.shape
    ssm, own = proj_out.shape[1], proj_in.shape[2]
    any_space = pl.BlockSpec(memory_space=pl.ANY)
    vmem = pl.BlockSpec(memory_space=pltpu.VMEM)
    slots = n - 1
    dma = pltpu.SemaphoreType.DMA
    return pl.pallas_call(
        functools.partial(kernel, n),
        out_shape=(
            jax.ShapeDtypeStruct(tokens.shape, tokens.dtype),
            jax.ShapeDtypeStruct(carried.shape, carried.dtype),
        ),
        in_specs=[any_space] * 6 + [vmem] * 6,
        out_specs=(any_space, any_space),
        scratch_shapes=[
            pltpu.VMEM((n, rows, width), BF16),
            pltpu.VMEM((n, ssm, width), BF16),
            pltpu.VMEM((n, own, rows), BF16),
            pltpu.VMEM((n, own, rows), BF16),
            pltpu.VMEM((n,) + norm_params.shape, BF16),
            pltpu.VMEM((n, 2, rows), F32),
            pltpu.VMEM(proj_in.shape, BF16),
            pltpu.VMEM(proj_in.shape, BF16),
            pltpu.VMEM(proj_in.shape[:2] + (2 * own,), BF16),
            pltpu.VMEM(proj_out.shape[1:], BF16),
            pltpu.VMEM(carried.shape, F32),
            pltpu.VMEM(carried.shape, F32),
            pltpu.VMEM((rows, 2 * own), F32),
            pltpu.VMEM((layers, groups, 2, state, 1), F32),
            pltpu.VMEM((layers, groups, 2 * state, own // groups), F32),
            pltpu.VMEM((rows, width), BF16),
            dma((4, slots)),
            dma((4, slots)),
            dma((n - 1,)),
            dma((n - 1,)),
            dma((n - 1,)),
            dma((n - 1,)),
            dma((10,)),
        ],
        compiler_params=pltpu.CompilerParams(
            collective_id=0, has_side_effects=True, vmem_limit_bytes=60 * 1024 * 1024
        ),
    )(*args)


def solution(mesh):
    return jax.shard_map(
        functools.partial(per_device, mesh.shape["tp"]),
        mesh=mesh,
        in_specs=(
            P("grp", "tp"),
            P(None, None, "tp", None, "grp"),
            P(None, None, "tp"),
            P(None, None, "tp"),
            P(None, None, "tp"),
            P(None, None, "tp"),
            P(None, "tp", None),
            P(None, "tp", None),
            P(None, "tp"),
            P(None, None, "tp", None, None),
            P(None, None, "tp", None, None),
            P(None, "tp"),
        ),
        out_specs=(P("grp", "tp"), P(None, None, "tp", None, "grp")),
        check_vma=False,
    )
```

```python
import functools

import jax
import jax.numpy as jnp
from jax import lax
from jax.experimental import pallas as pl
from jax.experimental.pallas import tpu as pltpu
from jax.sharding import PartitionSpec as P

RESIDUAL_SCALE = 1.4142135623730951
NORM_EPS = 1e-05
HIGHEST = lax.Precision.HIGHEST
F32 = jnp.float32
BF16 = jnp.bfloat16
VMEM_BYTES = 67043328


def column(row):
    m = row.shape[1]
    eye = lax.broadcasted_iota(jnp.int32, (m, m), 0) == lax.broadcasted_iota(jnp.int32, (m, m), 1)
    return jnp.sum(jnp.where(eye, jnp.broadcast_to(row, (m, m)), 0.0), axis=1, keepdims=True)


class Gather:
    def __init__(self, buf, send, recv, place, outer, part=None):
        self.part = part
        self.buf, self.send, self.recv, self.outer = buf, send, recv, outer
        self.z, self.y, self.c = place

    def idx(self, dz, dy, dc):
        z = lax.rem(self.z + dz + self.outer, self.outer)
        y = self.y if dy == 0 else 1 - self.y
        c = self.c if dc == 0 else 1 - self.c
        return (z * 2 + y) * 2 + c

    def copy(self, block, target, slot):
        ref = self.buf.at[block] if self.part is None else self.buf.at[block, self.part]
        return pltpu.make_async_remote_copy(
            src_ref=ref,
            dst_ref=ref,
            send_sem=self.send.at[slot],
            recv_sem=self.recv.at[slot],
            device_id={"tp": target},
            device_id_type=pl.DeviceIdType.MESH,
        )

    def out_z(self, dz):
        return self.copy(self.idx(0, 0, 0), self.idx(dz, 0, 0), dz - 1)

    def out_y(self, dz):
        return self.copy(self.idx(-dz, 0, 0), self.idx(0, 1, 0), self.outer - 1 + dz)

    def out_c(self, dz, dy):
        slot = 2 * self.outer - 1 + 2 * dz + dy
        return self.copy(self.idx(-dz, dy, 0), self.idx(0, 0, 1), slot)

    def start(self):
        self.out_y(0).start()
        for dz in range(1, self.outer):
            self.out_z(dz).start()
        self.out_c(0, 0).start()

    def arrive(self, dz, dy):
        if dy == 1:
            self.copy(self.idx(-dz, 1, 0), self.idx(0, 1, 0), self.outer - 1 + dz).wait_recv()
            self.out_c(dz, 1).start()
        elif dz > 0:
            self.copy(self.idx(-dz, 0, 0), self.idx(-dz, 0, 0), dz - 1).wait_recv()
            self.out_y(dz).start()
            self.out_c(dz, 0).start()

    def ready(self, dz, dy):
        slot = 2 * self.outer - 1 + 2 * dz + dy
        self.copy(self.idx(-dz, dy, 1), self.idx(0, 0, 1), slot).wait_recv()

    def sent(self):
        for dz in range(1, self.outer):
            self.out_z(dz).wait_send()
        for dz in range(self.outer):
            self.out_y(dz).wait_send()
            for dy in range(2):
                self.out_c(dz, dy).wait_send()

    def events(self):
        return [(dz, dy) for dz in range(self.outer) for dy in range(2)]

    def finish(self):
        for event in self.events():
            self.arrive(*event)
        for event in self.events():
            self.ready(*event)


def exchange(buf, send, recv, me, n, shift):
    return pltpu.make_async_remote_copy(
        src_ref=buf.at[me],
        dst_ref=buf.at[me],
        send_sem=send.at[shift - 1],
        recv_sem=recv.at[shift - 1],
        device_id={"tp": lax.rem(me + shift, n)},
        device_id_type=pl.DeviceIdType.MESH,
    )


def received(buf, send, recv, me, n, shift):
    block = lax.rem(me - shift + n, n)
    return pltpu.make_async_remote_copy(
        src_ref=buf.at[block],
        dst_ref=buf.at[block],
        send_sem=send.at[shift - 1],
        recv_sem=recv.at[shift - 1],
        device_id={"tp": block},
        device_id_type=pl.DeviceIdType.MESH,
    )


def kernel(
    n,
    tokens, carried, proj_in, proj_gate, proj_out, norm_params,
    lam_re_h, lam_im_h, log_step_h, in_c_h, out_c_h, skip_h,
    stream_out, new_carried,
    xg, pg, g1, g2, nb, sb, win, wgate, wcat, pown, states, fresh, acc, decay, bbar, outb,
    lam_re, lam_im, log_step, in_c, out_c, skip,
    gsend, grecv, nsend, nrecv, ssend, srecv, lsem,
):
    me = lax.axis_index("tp")
    outer = n // 4
    place = (me // 4, lax.rem(me // 2, 2), lax.rem(me, 2))
    layers, groups, state = lam_re.shape
    rows, width = tokens.shape
    ssm = proj_out.shape[1]
    own = proj_in.shape[1]
    ch = own // groups

    loads = [
        pltpu.make_async_copy(tokens, xg.at[me], lsem.at[0]),
        pltpu.make_async_copy(proj_out.at[0], pg.at[me], lsem.at[1]),
        pltpu.make_async_copy(norm_params, nb.at[me], lsem.at[2]),
        pltpu.make_async_copy(proj_in, win, lsem.at[3]),
        pltpu.make_async_copy(proj_gate, wgate, lsem.at[4]),
        pltpu.make_async_copy(carried, states, lsem.at[5]),
        pltpu.make_async_copy(proj_out.at[1], pown, lsem.at[6]),
    ]
    small = [(lam_re_h, lam_re), (lam_im_h, lam_im), (log_step_h, log_step), (in_c_h, in_c), (out_c_h, out_c), (skip_h, skip)]
    params = [pltpu.make_async_copy(a, b, lsem.at[10 + i]) for i, (a, b) in enumerate(small)]
    for load in loads[:5] + params + loads[5:]:
        load.start()
    barrier = pltpu.get_barrier_semaphore()
    for shift in range(1, n):
        pl.semaphore_signal(
            barrier, inc=1, device_id={"tp": lax.rem(me + shift, n)}, device_id_type=pl.DeviceIdType.MESH
        )
    pl.semaphore_wait(barrier, n - 1)

    half = rows // 2
    halves = [
        Gather(xg, gsend.at[k], grecv.at[k], place, outer, pl.ds(part * half, half))
        for part, k in enumerate((0, 4))
    ]
    gp = Gather(pg, gsend.at[1], grecv.at[1], place, outer)
    gg = [Gather(g1, gsend.at[2], grecv.at[2], place, outer), Gather(g2, gsend.at[3], grecv.at[3], place, outer)]
    loads[0].wait()
    for ga in halves:
        ga.start()
    loads[2].wait()
    for shift in range(1, n):
        exchange(nb, nsend, nrecv, me, n, shift).start()
    loads[1].wait()
    gp.start()

    loads[3].wait()
    loads[4].wait()
    for load in params:
        load.wait()
    for l in range(layers):
        wcat[l] = jnp.concatenate([win[l], wgate[l]], axis=0).astype(F32).T.astype(BF16)
    for l in range(layers):
        for g in range(groups):
            lr = lam_re[l, g : g + 1, :]
            li = lam_im[l, g : g + 1, :]
            step_len = jnp.exp(log_step[l : l + 1, g : g + 1])
            modulus = jnp.exp(lr * step_len)
            d_re = modulus * jnp.cos(li * step_len)
            d_im = modulus * jnp.sin(li * step_len)
            den = lr * lr + li * li
            shifted = d_re - 1.0
            k_re = (shifted * lr + d_im * li) / den
            k_im = (d_im * lr - shifted * li) / den
            decay[l, g, 0] = column(d_re)
            decay[l, g, 1] = column(d_im)
            bbar[l, g, :state] = (k_re * in_c[l, 0, g] - k_im * in_c[l, 1, g]).T
            bbar[l, g, state:] = (k_re * in_c[l, 1, g] + k_im * in_c[l, 0, g]).T

    def pair_dot(ga, dz, dy, first):
        j = ga.idx(-dz, dy, 0) // 2
        lhs = jnp.concatenate([xg[2 * j, ga.part, :], xg[2 * j + 1, ga.part, :]], axis=1)
        rhs = wcat[0, pl.ds(pl.multiple_of(j * (2 * width), 2 * width), 2 * width), :]
        part = jnp.dot(lhs, rhs, preferred_element_type=F32)
        if first:
            acc[ga.part, :] = part
        else:
            acc[ga.part, :] += part

    due = None
    for ga in halves:
        for i, event in enumerate(ga.events()):
            ga.arrive(*event)
            if due is not None:
                due[0].ready(*due[1])
                pair_dot(due[0], *due[1], due[2])
            due = (ga, event, i == 0)
    due[0].ready(*due[1])
    pair_dot(due[0], *due[1], due[2])

    def mixer(l, gbuf, between):
        pre_t = acc[...].astype(BF16).astype(F32).T
        skip_col = column(skip[l : l + 1, :])
        parts = []
        for g in range(groups):
            drive = pre_t[g * ch : (g + 1) * ch]
            push = jnp.dot(bbar[l, g], drive, precision=HIGHEST, preferred_element_type=F32)
            old_re, old_im = states[l, 0, g], states[l, 1, g]
            d_re, d_im = decay[l, g, 0], decay[l, g, 1]
            new_re = d_re * old_re - d_im * old_im + push[:state]
            new_im = d_re * old_im + d_im * old_re + push[state:]
            fresh[l, 0, g] = new_re
            fresh[l, 1, g] = new_im
            parts.append(
                jnp.dot(out_c[l, 0, g], new_re, precision=HIGHEST, preferred_element_type=F32)
                - jnp.dot(out_c[l, 1, g], new_im, precision=HIGHEST, preferred_element_type=F32)
                + skip_col[g * ch : (g + 1) * ch] * drive
            )
            between(g)
        y = jnp.concatenate(parts, axis=0) if groups > 1 else parts[0]
        gbuf[me] = (jax.nn.gelu(y) * jax.nn.sigmoid(pre_t[own:])).astype(BF16)

    p_events = gp.events()
    for event in p_events[: len(p_events) // 4]:
        gp.arrive(*event)
    loads[5].wait()

    def p_step(g):
        share = len(p_events) // 4
        if g == 0:
            for event in p_events[share : 2 * share]:
                gp.arrive(*event)

    mixer(0, g1, p_step)
    gg[0].start()
    stores = [pltpu.make_async_copy(fresh.at[0], new_carried.at[0], lsem.at[7])]
    stores[0].start()
    for event in p_events[len(p_events) // 4 * 2 :]:
        gp.arrive(*event)
    for event in p_events:
        gp.ready(*event)
    gg[0].finish()
    for shift in range(1, n):
        received(nb, nsend, nrecv, me, n, shift).wait_recv()
    for ga in halves:
        ga.sent()

    chunk = min(rows, 128)

    def row_chunk(r, carry):
        at = pl.ds(pl.multiple_of(r * chunk, chunk), chunk)
        gated = g1[:, :, at].reshape(ssm, chunk).astype(F32).T.astype(BF16)
        total = jnp.zeros((chunk, 1), F32)
        square = jnp.zeros((chunk, 1), F32)
        wide = []
        for j in range(n // 2):
            weights = jnp.concatenate([pg[2 * j], pg[2 * j + 1]], axis=1)
            mixed = jnp.dot(gated, weights, preferred_element_type=F32)
            old = jnp.concatenate([xg[2 * j, at, :], xg[2 * j + 1, at, :]], axis=1)
            summed = (RESIDUAL_SCALE * old.astype(F32) + mixed).astype(BF16)
            s = summed.astype(F32)
            total += jnp.sum(s, axis=1, keepdims=True)
            square += jnp.sum(s * s, axis=1, keepdims=True)
            wide.append(summed)
        mean = total / (n * width)
        var = square / (n * width) - mean * mean
        scale = lax.rsqrt(var + NORM_EPS)
        pre = jnp.zeros((chunk, 2 * own), F32)
        for j in range(n // 2):
            par = jnp.concatenate([nb[2 * j, 0], nb[2 * j + 1, 0]], axis=1).astype(F32)
            out = ((wide[j].astype(F32) - mean) * scale * par[0:1] + par[1:2]).astype(BF16)
            xg[2 * j, at, :] = out[:, :width]
            xg[2 * j + 1, at, :] = out[:, width:]
            pre += jnp.dot(out, wcat[1, 2 * j * width : 2 * (j + 1) * width, :], preferred_element_type=F32)
        acc[at, :] = pre
        return carry

    lax.fori_loop(0, rows // chunk, row_chunk, 0)

    mixer(1, g2, lambda g: None)
    gg[1].start()
    stores.append(pltpu.make_async_copy(fresh.at[1], new_carried.at[1], lsem.at[8]))
    stores[1].start()
    residual_t = RESIDUAL_SCALE * xg[me].astype(F32).T
    gain = column(nb[me, 1].astype(F32)[0:1])
    bias = column(nb[me, 1].astype(F32)[1:2])
    loads[6].wait()
    weights_t = pown[...].astype(F32).T.astype(BF16)
    gg[1].finish()
    mixed_t = jnp.dot(weights_t, g2[...].reshape(ssm, rows), preferred_element_type=F32)
    s = (residual_t + mixed_t).astype(BF16).astype(F32)
    sb[me] = jnp.concatenate([jnp.sum(s, axis=0, keepdims=True), jnp.sum(s * s, axis=0, keepdims=True)], axis=0)
    for shift in range(1, n):
        exchange(sb, ssend, srecv, me, n, shift).start()
    for shift in range(1, n):
        received(sb, ssend, srecv, me, n, shift).wait_recv()
    sums = jnp.sum(sb[...], axis=0) / (n * width)
    mean = sums[0:1]
    scale = lax.rsqrt(sums[1:2] - mean * mean + NORM_EPS)
    outb[...] = ((s - mean) * scale * gain + bias).T.astype(BF16)
    last = pltpu.make_async_copy(outb, stream_out, lsem.at[9])
    last.start()
    for gather in (gp, gg[0], gg[1]):
        gather.sent()
    for shift in range(1, n):
        exchange(nb, nsend, nrecv, me, n, shift).wait_send()
        exchange(sb, ssend, srecv, me, n, shift).wait_send()
    for store in stores:
        store.wait()
    last.wait()


def deliver(stream, fresh, stream_out, new_carried, sem):
    copies = [pltpu.make_async_copy(stream, stream_out, sem.at[0]), pltpu.make_async_copy(fresh, new_carried, sem.at[1])]
    for copy in copies:
        copy.start()
    for copy in copies:
        copy.wait()


def per_device(n, *args):
    args = list(args)
    for i in (2, 3, 9):
        args[i] = jnp.swapaxes(args[i], -1, -2)
    tokens, carried, proj_in, _, proj_out, norm_params, lam_re = args[:7]
    rows, width = tokens.shape
    layers, groups, state = lam_re.shape
    ssm, own = proj_out.shape[1], proj_in.shape[1]
    any_space = pl.BlockSpec(memory_space=pl.ANY)
    slots = n - 1
    delivered = carried.size * 4 + rows * max(width, 128) * 2
    dma = pltpu.SemaphoreType.DMA
    stream, fresh = pl.pallas_call(
        functools.partial(kernel, n),
        out_shape=(
            pltpu.VMEM(tokens.shape, tokens.dtype),
            pltpu.VMEM(carried.shape, carried.dtype),
        ),
        in_specs=[pl.BlockSpec(memory_space=pltpu.HBM)] * len(args),
        out_specs=(any_space, any_space),
        scratch_shapes=[
            pltpu.VMEM((n, rows, width), BF16),
            pltpu.VMEM((n, ssm, width), BF16),
            pltpu.VMEM((n, own, rows), BF16),
            pltpu.VMEM((n, own, rows), BF16),
            pltpu.VMEM((n,) + norm_params.shape, BF16),
            pltpu.VMEM((n, 2, rows), F32),
            pltpu.VMEM(proj_in.shape, BF16),
            pltpu.VMEM(proj_in.shape, BF16),
            pltpu.VMEM((layers, n * width, 2 * own), BF16),
            pltpu.VMEM(proj_out.shape[1:], BF16),
            pltpu.VMEM(carried.shape, F32),
            pltpu.VMEM(carried.shape, F32),
            pltpu.VMEM((rows, 2 * own), F32),
            pltpu.VMEM((layers, groups, 2, state, 1), F32),
            pltpu.VMEM((layers, groups, 2 * state, own // groups), F32),
            pltpu.VMEM((rows, width), BF16),
            *[pltpu.VMEM(a.shape, a.dtype) for a in args[6:]],
            dma((5, slots)),
            dma((5, slots)),
            dma((n - 1,)),
            dma((n - 1,)),
            dma((n - 1,)),
            dma((n - 1,)),
            dma((10 + len(args) - 6,)),
        ],
        compiler_params=pltpu.CompilerParams(
            collective_id=0, has_side_effects=True, vmem_limit_bytes=VMEM_BYTES - delivered - (1 << 18)
        ),
    )(*args)
    return pl.pallas_call(
        deliver,
        out_shape=(
            jax.ShapeDtypeStruct(tokens.shape, tokens.dtype),
            jax.ShapeDtypeStruct(carried.shape, carried.dtype),
        ),
        in_specs=[any_space] * 2,
        out_specs=(any_space, any_space),
        scratch_shapes=[dma((2,))],
        compiler_params=pltpu.CompilerParams(vmem_limit_bytes=1024 * 1024),
    )(stream, fresh)


def solution(mesh):
    return jax.shard_map(
        functools.partial(per_device, mesh.shape["tp"]),
        mesh=mesh,
        in_specs=(
            P("grp", "tp"),
            P(None, None, "tp", None, "grp"),
            P(None, None, "tp"),
            P(None, None, "tp"),
            P(None, None, "tp"),
            P(None, None, "tp"),
            P(None, "tp", None),
            P(None, "tp", None),
            P(None, "tp"),
            P(None, None, "tp", None, None),
            P(None, None, "tp", None, None),
            P(None, "tp"),
        ),
        out_specs=(P("grp", "tp"), P(None, None, "tp", None, "grp")),
        check_vma=False,
    )
```

```python
import functools

import jax
import jax.numpy as jnp
from jax import lax
from jax.experimental import pallas as pl
from jax.experimental.pallas import tpu as pltpu
from jax.sharding import PartitionSpec as P

RESIDUAL_SCALE = 1.4142135623730951
NORM_EPS = 1e-05
HIGHEST = lax.Precision.HIGHEST
F32 = jnp.float32
BF16 = jnp.bfloat16
VMEM_BYTES = 67043328


def column(row):
    m = row.shape[1]
    eye = lax.broadcasted_iota(jnp.int32, (m, m), 0) == lax.broadcasted_iota(jnp.int32, (m, m), 1)
    return jnp.sum(jnp.where(eye, jnp.broadcast_to(row, (m, m)), 0.0), axis=1, keepdims=True)


class Gather:
    def __init__(self, buf, send, recv, place, outer, part=None):
        self.part = part
        self.buf, self.send, self.recv, self.outer = buf, send, recv, outer
        self.z, self.y, self.c = place

    def idx(self, dz, dy, dc):
        z = lax.rem(self.z + dz + self.outer, self.outer)
        y = self.y if dy == 0 else 1 - self.y
        c = self.c if dc == 0 else 1 - self.c
        return (z * 2 + y) * 2 + c

    def copy(self, block, target, slot):
        ref = self.buf.at[block] if self.part is None else self.buf.at[block, self.part]
        return pltpu.make_async_remote_copy(
            src_ref=ref,
            dst_ref=ref,
            send_sem=self.send.at[slot],
            recv_sem=self.recv.at[slot],
            device_id={"tp": target},
            device_id_type=pl.DeviceIdType.MESH,
        )

    def out_z(self, dz):
        return self.copy(self.idx(0, 0, 0), self.idx(dz, 0, 0), dz - 1)

    def out_y(self, dz):
        return self.copy(self.idx(-dz, 0, 0), self.idx(0, 1, 0), self.outer - 1 + dz)

    def out_c(self, dz, dy):
        slot = 2 * self.outer - 1 + 2 * dz + dy
        return self.copy(self.idx(-dz, dy, 0), self.idx(0, 0, 1), slot)

    def start(self):
        self.out_y(0).start()
        for dz in range(1, self.outer):
            self.out_z(dz).start()
        self.out_c(0, 0).start()

    def arrive(self, dz, dy):
        if dy == 1:
            self.copy(self.idx(-dz, 1, 0), self.idx(0, 1, 0), self.outer - 1 + dz).wait_recv()
            self.out_c(dz, 1).start()
        elif dz > 0:
            self.copy(self.idx(-dz, 0, 0), self.idx(-dz, 0, 0), dz - 1).wait_recv()
            self.out_y(dz).start()
            self.out_c(dz, 0).start()

    def ready(self, dz, dy):
        slot = 2 * self.outer - 1 + 2 * dz + dy
        self.copy(self.idx(-dz, dy, 1), self.idx(0, 0, 1), slot).wait_recv()

    def sent(self):
        for dz in range(1, self.outer):
            self.out_z(dz).wait_send()
        for dz in range(self.outer):
            self.out_y(dz).wait_send()
            for dy in range(2):
                self.out_c(dz, dy).wait_send()

    def events(self):
        return [(dz, dy) for dz in range(self.outer) for dy in range(2)]

    def finish(self):
        for event in self.events():
            self.arrive(*event)
        for event in self.events():
            self.ready(*event)


def exchange(buf, send, recv, me, n, shift):
    return pltpu.make_async_remote_copy(
        src_ref=buf.at[me],
        dst_ref=buf.at[me],
        send_sem=send.at[shift - 1],
        recv_sem=recv.at[shift - 1],
        device_id={"tp": lax.rem(me + shift, n)},
        device_id_type=pl.DeviceIdType.MESH,
    )


def received(buf, send, recv, me, n, shift):
    block = lax.rem(me - shift + n, n)
    return pltpu.make_async_remote_copy(
        src_ref=buf.at[block],
        dst_ref=buf.at[block],
        send_sem=send.at[shift - 1],
        recv_sem=recv.at[shift - 1],
        device_id={"tp": block},
        device_id_type=pl.DeviceIdType.MESH,
    )


def kernel(
    n,
    tokens, carried, proj_in, proj_gate, proj_out, norm_params,
    lam_re_h, lam_im_h, log_step_h, in_c_h, out_c_h, skip_h,
    stream_out, new_carried,
    xg, pg, g1, g2, nb, sb, win, wgate, wcat, pown, states, fresh, acc, decay, bbar, outb,
    lam_re, lam_im, log_step, in_c, out_c, skip,
    gsend, grecv, nsend, nrecv, ssend, srecv, lsem,
):
    me = lax.axis_index("tp")
    outer = n // 4
    place = (me // 4, lax.rem(me // 2, 2), lax.rem(me, 2))
    layers, groups, state = lam_re.shape
    rows, width = tokens.shape
    ssm = proj_out.shape[1]
    own = proj_in.shape[1]
    ch = own // groups

    loads = [
        pltpu.make_async_copy(tokens, xg.at[me], lsem.at[0]),
        pltpu.make_async_copy(proj_out.at[0], pg.at[me], lsem.at[1]),
        pltpu.make_async_copy(norm_params, nb.at[me], lsem.at[2]),
        pltpu.make_async_copy(proj_in, win, lsem.at[3]),
        pltpu.make_async_copy(proj_gate, wgate, lsem.at[4]),
        pltpu.make_async_copy(carried, states, lsem.at[5]),
        pltpu.make_async_copy(proj_out.at[1], pown, lsem.at[6]),
    ]
    small = [(lam_re_h, lam_re), (lam_im_h, lam_im), (log_step_h, log_step), (in_c_h, in_c), (out_c_h, out_c), (skip_h, skip)]
    params = [pltpu.make_async_copy(a, b, lsem.at[10 + i]) for i, (a, b) in enumerate(small)]
    for load in loads[:5] + params + loads[5:]:
        load.start()
    barrier = pltpu.get_barrier_semaphore()
    for shift in range(1, n):
        pl.semaphore_signal(
            barrier, inc=1, device_id={"tp": lax.rem(me + shift, n)}, device_id_type=pl.DeviceIdType.MESH
        )
    pl.semaphore_wait(barrier, n - 1)

    half = rows // 2
    halves = [
        Gather(xg, gsend.at[k], grecv.at[k], place, outer, pl.ds(part * half, half))
        for part, k in enumerate((0, 4))
    ]
    gp = Gather(pg, gsend.at[1], grecv.at[1], place, outer)
    g_in = [Gather(g1.at[h], gsend.at[2 + h], grecv.at[2 + h], place, outer) for h in range(2)]
    g_out = [Gather(g2.at[h], gsend.at[5 + h], grecv.at[5 + h], place, outer) for h in range(2)]
    loads[0].wait()
    for ga in halves:
        ga.start()
    loads[2].wait()
    for shift in range(1, n):
        exchange(nb, nsend, nrecv, me, n, shift).start()
    loads[1].wait()
    gp.start()

    loads[3].wait()
    loads[4].wait()
    for load in params:
        load.wait()
    for l in range(layers):
        wcat[l] = jnp.concatenate([win[l], wgate[l]], axis=0).astype(F32).T.astype(BF16)
    for l in range(layers):
        for g in range(groups):
            lr = lam_re[l, g : g + 1, :]
            li = lam_im[l, g : g + 1, :]
            step_len = jnp.exp(log_step[l : l + 1, g : g + 1])
            modulus = jnp.exp(lr * step_len)
            d_re = modulus * jnp.cos(li * step_len)
            d_im = modulus * jnp.sin(li * step_len)
            den = lr * lr + li * li
            shifted = d_re - 1.0
            k_re = (shifted * lr + d_im * li) / den
            k_im = (d_im * lr - shifted * li) / den
            decay[l, g, 0] = column(d_re)
            decay[l, g, 1] = column(d_im)
            bbar[l, g, :state] = (k_re * in_c[l, 0, g] - k_im * in_c[l, 1, g]).T
            bbar[l, g, state:] = (k_re * in_c[l, 1, g] + k_im * in_c[l, 0, g]).T

    def pair_dot(ga, dz, dy, first):
        j = ga.idx(-dz, dy, 0) // 2
        lhs = jnp.concatenate([xg[2 * j, ga.part, :], xg[2 * j + 1, ga.part, :]], axis=1)
        rhs = wcat[0, pl.ds(pl.multiple_of(j * (2 * width), 2 * width), 2 * width), :]
        part = jnp.dot(lhs, rhs, preferred_element_type=F32)
        if first:
            acc[ga.part, :] = part
        else:
            acc[ga.part, :] += part

    def token_half(ga):
        due = None
        for i, event in enumerate(ga.events()):
            ga.arrive(*event)
            if due is not None:
                ga.ready(*due)
                pair_dot(ga, *due, i == 1)
            due = event
        ga.ready(*due)
        pair_dot(ga, *due, False)

    def mixer(l, gbuf, h):
        at = pl.ds(h * half, half)
        pre_t = acc[at, :].astype(BF16).astype(F32).T
        skip_col = column(skip[l : l + 1, :])
        parts = []
        for g in range(groups):
            drive = pre_t[g * ch : (g + 1) * ch]
            push = jnp.dot(bbar[l, g], drive, precision=HIGHEST, preferred_element_type=F32)
            old_re, old_im = states[l, 0, g, :, at], states[l, 1, g, :, at]
            d_re, d_im = decay[l, g, 0], decay[l, g, 1]
            new_re = d_re * old_re - d_im * old_im + push[:state]
            new_im = d_re * old_im + d_im * old_re + push[state:]
            fresh[l, 0, g, :, at] = new_re
            fresh[l, 1, g, :, at] = new_im
            parts.append(
                jnp.dot(out_c[l, 0, g], new_re, precision=HIGHEST, preferred_element_type=F32)
                - jnp.dot(out_c[l, 1, g], new_im, precision=HIGHEST, preferred_element_type=F32)
                + skip_col[g * ch : (g + 1) * ch] * drive
            )
        y = jnp.concatenate(parts, axis=0) if groups > 1 else parts[0]
        gbuf[h, me] = (jax.nn.gelu(y) * jax.nn.sigmoid(pre_t[own:])).astype(BF16)

    token_half(halves[0])
    loads[5].wait()
    mixer(0, g1, 0)
    g_in[0].start()
    token_half(halves[1])
    p_events = gp.events()
    for event in p_events[: len(p_events) // 2]:
        gp.arrive(*event)
    mixer(0, g1, 1)
    g_in[1].start()
    stores = [pltpu.make_async_copy(fresh.at[0], new_carried.at[0], lsem.at[7])]
    stores[0].start()
    for event in p_events[len(p_events) // 2 :]:
        gp.arrive(*event)
    for event in g_in[0].events():
        g_in[0].arrive(*event)
    for event in p_events:
        gp.ready(*event)
    for event in g_in[0].events():
        g_in[0].ready(*event)
    for shift in range(1, n):
        received(nb, nsend, nrecv, me, n, shift).wait_recv()
    for ga in halves:
        ga.sent()

    chunk = min(half, 128)

    def row_chunk(h, r, carry):
        at = pl.ds(pl.multiple_of(h * half + r * chunk, chunk), chunk)
        gated = g1[h, :, :, pl.ds(pl.multiple_of(r * chunk, chunk), chunk)].reshape(ssm, chunk).astype(F32).T.astype(BF16)
        total = jnp.zeros((chunk, 1), F32)
        square = jnp.zeros((chunk, 1), F32)
        wide = []
        for j in range(n // 2):
            weights = jnp.concatenate([pg[2 * j], pg[2 * j + 1]], axis=1)
            mixed = jnp.dot(gated, weights, preferred_element_type=F32)
            old = jnp.concatenate([xg[2 * j, at, :], xg[2 * j + 1, at, :]], axis=1)
            summed = (RESIDUAL_SCALE * old.astype(F32) + mixed).astype(BF16)
            s = summed.astype(F32)
            total += jnp.sum(s, axis=1, keepdims=True)
            square += jnp.sum(s * s, axis=1, keepdims=True)
            wide.append(summed)
        mean = total / (n * width)
        var = square / (n * width) - mean * mean
        scale = lax.rsqrt(var + NORM_EPS)
        pre = jnp.zeros((chunk, 2 * own), F32)
        for j in range(n // 2):
            par = jnp.concatenate([nb[2 * j, 0], nb[2 * j + 1, 0]], axis=1).astype(F32)
            out = ((wide[j].astype(F32) - mean) * scale * par[0:1] + par[1:2]).astype(BF16)
            xg[2 * j, at, :] = out[:, :width]
            xg[2 * j + 1, at, :] = out[:, width:]
            pre += jnp.dot(out, wcat[1, 2 * j * width : 2 * (j + 1) * width, :], preferred_element_type=F32)
        acc[at, :] = pre
        return carry

    lax.fori_loop(0, half // chunk, functools.partial(row_chunk, 0), 0)
    mixer(1, g2, 0)
    g_out[0].start()
    g_in[1].finish()
    lax.fori_loop(0, half // chunk, functools.partial(row_chunk, 1), 0)
    mixer(1, g2, 1)
    g_out[1].start()
    stores.append(pltpu.make_async_copy(fresh.at[1], new_carried.at[1], lsem.at[8]))
    stores[1].start()
    residual_t = RESIDUAL_SCALE * xg[me].astype(F32).T
    gain = column(nb[me, 1].astype(F32)[0:1])
    bias = column(nb[me, 1].astype(F32)[1:2])
    loads[6].wait()
    weights_t = pown[...].astype(F32).T.astype(BF16)
    sums = []
    for h in range(2):
        g_out[h].finish()
        mixed_t = jnp.dot(weights_t, g2[h].reshape(ssm, half), preferred_element_type=F32)
        sums.append((residual_t[:, h * half : (h + 1) * half] + mixed_t).astype(BF16).astype(F32))
    s = jnp.concatenate(sums, axis=1)
    sb[me] = jnp.concatenate([jnp.sum(s, axis=0, keepdims=True), jnp.sum(s * s, axis=0, keepdims=True)], axis=0)
    for shift in range(1, n):
        exchange(sb, ssend, srecv, me, n, shift).start()
    for shift in range(1, n):
        received(sb, ssend, srecv, me, n, shift).wait_recv()
    sums = jnp.sum(sb[...], axis=0) / (n * width)
    mean = sums[0:1]
    scale = lax.rsqrt(sums[1:2] - mean * mean + NORM_EPS)
    outb[...] = ((s - mean) * scale * gain + bias).T.astype(BF16)
    last = pltpu.make_async_copy(outb, stream_out, lsem.at[9])
    last.start()
    for gather in (gp, *g_in, *g_out):
        gather.sent()
    for shift in range(1, n):
        exchange(nb, nsend, nrecv, me, n, shift).wait_send()
        exchange(sb, ssend, srecv, me, n, shift).wait_send()
    for store in stores:
        store.wait()
    last.wait()


def deliver(stream, fresh, stream_out, new_carried, sem):
    copies = [pltpu.make_async_copy(stream, stream_out, sem.at[0]), pltpu.make_async_copy(fresh, new_carried, sem.at[1])]
    for copy in copies:
        copy.start()
    for copy in copies:
        copy.wait()


def per_device(n, *args):
    args = list(args)
    for i in (2, 3, 9):
        args[i] = jnp.swapaxes(args[i], -1, -2)
    tokens, carried, proj_in, _, proj_out, norm_params, lam_re = args[:7]
    rows, width = tokens.shape
    layers, groups, state = lam_re.shape
    ssm, own = proj_out.shape[1], proj_in.shape[1]
    any_space = pl.BlockSpec(memory_space=pl.ANY)
    slots = n - 1
    delivered = carried.size * 4 + rows * max(width, 128) * 2
    dma = pltpu.SemaphoreType.DMA
    stream, fresh = pl.pallas_call(
        functools.partial(kernel, n),
        out_shape=(
            pltpu.VMEM(tokens.shape, tokens.dtype),
            pltpu.VMEM(carried.shape, carried.dtype),
        ),
        in_specs=[pl.BlockSpec(memory_space=pltpu.HBM)] * len(args),
        out_specs=(any_space, any_space),
        scratch_shapes=[
            pltpu.VMEM((n, rows, width), BF16),
            pltpu.VMEM((n, ssm, width), BF16),
            pltpu.VMEM((2, n, own, rows // 2), BF16),
            pltpu.VMEM((2, n, own, rows // 2), BF16),
            pltpu.VMEM((n,) + norm_params.shape, BF16),
            pltpu.VMEM((n, 2, rows), F32),
            pltpu.VMEM(proj_in.shape, BF16),
            pltpu.VMEM(proj_in.shape, BF16),
            pltpu.VMEM((layers, n * width, 2 * own), BF16),
            pltpu.VMEM(proj_out.shape[1:], BF16),
            pltpu.VMEM(carried.shape, F32),
            pltpu.VMEM(carried.shape, F32),
            pltpu.VMEM((rows, 2 * own), F32),
            pltpu.VMEM((layers, groups, 2, state, 1), F32),
            pltpu.VMEM((layers, groups, 2 * state, own // groups), F32),
            pltpu.VMEM((rows, width), BF16),
            *[pltpu.VMEM(a.shape, a.dtype) for a in args[6:]],
            dma((7, slots)),
            dma((7, slots)),
            dma((n - 1,)),
            dma((n - 1,)),
            dma((n - 1,)),
            dma((n - 1,)),
            dma((10 + len(args) - 6,)),
        ],
        compiler_params=pltpu.CompilerParams(
            collective_id=0, has_side_effects=True, vmem_limit_bytes=VMEM_BYTES - delivered - (1 << 18)
        ),
    )(*args)
    return pl.pallas_call(
        deliver,
        out_shape=(
            jax.ShapeDtypeStruct(tokens.shape, tokens.dtype),
            jax.ShapeDtypeStruct(carried.shape, carried.dtype),
        ),
        in_specs=[any_space] * 2,
        out_specs=(any_space, any_space),
        scratch_shapes=[dma((2,))],
        compiler_params=pltpu.CompilerParams(vmem_limit_bytes=1024 * 1024),
    )(stream, fresh)


def solution(mesh):
    return jax.shard_map(
        functools.partial(per_device, mesh.shape["tp"]),
        mesh=mesh,
        in_specs=(
            P("grp", "tp"),
            P(None, None, "tp", None, "grp"),
            P(None, None, "tp"),
            P(None, None, "tp"),
            P(None, None, "tp"),
            P(None, None, "tp"),
            P(None, "tp", None),
            P(None, "tp", None),
            P(None, "tp"),
            P(None, None, "tp", None, None),
            P(None, None, "tp", None, None),
            P(None, "tp"),
        ),
        out_specs=(P("grp", "tp"), P(None, None, "tp", None, "grp")),
        check_vma=False,
    )
```
